32 devices in a mesh: fs: 4 (over y, x), tp: 8 (over z, core).
Axes of the slice: x: 2, y: 2, z: 4, core: 2. Of those that a mesh axis runs over, the one named last changes fastest.
Arguments:
- saved_input: bfloat16 [4096, 4096], P('fs', 'tp'), may hold values from -6 to 6
- query_cot: bfloat16 [4096, 4096], P('fs', 'tp'), may hold values from -6 to 6
- key_cot: bfloat16 [4096, 4096], P('fs', 'tp'), may hold values from -6 to 6
- query_master: float32 [4096, 4096], P('fs', 'tp'), may hold values from -0.09375 to 0.09375
- key_master: float32 [4096, 4096], P('fs', 'tp'), may hold values from -0.09375 to 0.09375
- query_basis: bfloat16 [4096, 256], P('fs'), may hold values from -3 to 3
- key_basis: bfloat16 [4096, 256], P('fs'), may hold values from -3 to 3
- query_first: float32 [256, 4096], P('fs', 'tp'), may hold values from -240 to 240
- query_second: float32 [256, 4096], P('fs', 'tp'), may hold values from 1000 to 20000
- key_first: float32 [256, 4096], P('fs', 'tp'), may hold values from -240 to 240
- key_second: float32 [256, 4096], P('fs', 'tp'), may hold values from 1000 to 20000
Outputs:
- query_step: float32 [4096, 4096], P('fs', 'tp')
- query_weight: float32 [4096, 4096], P('fs', 'tp')
- query_copy: bfloat16 [4096, 4096], P(None, 'tp')
- query_first_new: float32 [256, 4096], P('fs', 'tp')
- query_second_new: float32 [256, 4096], P('fs', 'tp')
- key_step: float32 [4096, 4096], P('fs', 'tp')
- key_weight: float32 [4096, 4096], P('fs', 'tp')
- key_copy: bfloat16 [4096, 4096], P(None, 'tp')
- key_first_new: float32 [256, 4096], P('fs', 'tp')
- key_second_new: float32 [256, 4096], P('fs', 'tp')
The draws below stay inside these ranges and needn't reach their ends.
All inputs are finite; a program needn't handle non-finite values.
Results may differ from the reference program's by a relative error of at most 0.0065.
Values may be sent and summed in bfloat16 or wider, within the bound.
A program may use at most 64 MiB of HBM per device.

```python
import math
import jax
import jax.numpy as jnp
from jax import lax

D = 4096
HEADS = 32
HD = 128
RANK = 256
TOKENS = 4096


def basis_draw(key, salt):
    base = jax.random.fold_in(key, salt)
    entry_key, factor_key = jax.random.split(base)
    group = max(D // 64, 1)
    groups = D // group
    entries = jnp.clip(jax.random.normal(entry_key, (D, RANK), jnp.float32), -4.0, 4.0)
    factors = jnp.exp(jax.random.uniform(factor_key, (groups,), jnp.float32, -1.5, 1.5))
    row_scale = jnp.repeat(factors, group)
    values = entries * row_scale[:, None] * D ** (-0.5)
    return values.astype(jnp.bfloat16)


def draw_query_basis(key, part):
    return basis_draw(key, 101)


def draw_key_basis(key, part):
    return basis_draw(key, 202)


def block_scale(key, dims, pieces, low, largest):
    loudness, own = 1.0, jax.random.fold_in(key, 6)
    for position, blocks in pieces:
        steps = jnp.exp(jax.random.uniform(jax.random.fold_in(own, position), (blocks,), jnp.float32, low / len(pieces), largest / len(pieces)))
        loudness = loudness * jnp.repeat(steps, dims[position] // blocks).reshape([-1 if axis == position else 1 for axis in range(len(dims))])
    return loudness


def bell_draw(stream_key, shape, scale, most, cuts=(), kind=jnp.bfloat16):
    values = jax.random.normal(stream_key, shape, jnp.float32) * scale
    if len(cuts) > 0:
        values = block_scale(stream_key, shape, cuts, -0.22, 0.18) * values
    return jnp.clip(values, min=-most, max=most).astype(kind)


def setup_inputs(seed: int = 0) -> dict:
    seeds = jax.random.split(jax.random.key(seed), 12)
    saved_input = bell_draw(seeds[0], (TOKENS, D), 1.0, 6.0, ((0, 4), (1, 8)))
    query_cot = bell_draw(seeds[1], (TOKENS, HEADS * HD), 1.0, 6.0, ((0, 4), (1, 8)))
    key_cot = bell_draw(seeds[2], (TOKENS, HEADS * HD), 1.0, 6.0, ((0, 4), (1, 8)))
    query_master = bell_draw(seeds[3], (D, HEADS * HD), D ** -0.5, 0.09375, ((0, 4), (1, 8)), jnp.float32)
    key_master = bell_draw(seeds[4], (D, HEADS * HD), D ** -0.5, 0.09375, ((0, 4), (1, 8)), jnp.float32)
    query_basis = draw_query_basis(jax.random.fold_in(seeds[11], 71), 0)
    key_basis = draw_key_basis(jax.random.fold_in(seeds[11], 71), 0)
    query_first = bell_draw(seeds[7], (RANK, HEADS * HD), 40.0, 240.0, ((0, 4), (1, 8)), jnp.float32)
    query_second = jnp.clip(jnp.exp(math.log(20000.0) - 2.9957323 * jax.random.uniform(seeds[8], (RANK, HEADS * HD), jnp.float32) ** block_scale(seeds[8], (RANK, HEADS * HD), ((0, 4), (1, 8)), -0.2, 0.2)), 1000.0, 20000.0)
    key_first = bell_draw(seeds[9], (RANK, HEADS * HD), 40.0, 240.0, ((0, 4), (1, 8)), jnp.float32)
    key_second = jnp.clip(jnp.exp(math.log(20000.0) - 2.9957323 * jax.random.uniform(seeds[10], (RANK, HEADS * HD), jnp.float32) ** block_scale(seeds[10], (RANK, HEADS * HD), ((0, 4), (1, 8)), -0.2, 0.2)), 1000.0, 20000.0)
    return {"saved_input": saved_input, "query_cot": query_cot, "key_cot": key_cot, "query_master": query_master, "key_master": key_master, "query_basis": query_basis, "key_basis": key_basis, "query_first": query_first, "query_second": query_second, "key_first": key_first, "key_second": key_second}


moment_decay = 0.8
square_decay = 0.9
square_floor = 1.0
norm_floor = 0.01
step_rate = 0.01

def update_one(saved_input, cotangent, master, basis, first, second):
    grad = jnp.dot(saved_input.T, cotangent, preferred_element_type=jnp.float32)
    low = jnp.dot(basis.astype(jnp.float32).T, grad, precision=lax.Precision.HIGHEST)
    first_new = moment_decay * first + (1.0 - moment_decay) * low
    second_new = square_decay * second + (1.0 - square_decay) * low * low
    ratio = (first_new / jnp.sqrt(second_new + square_floor)).astype(jnp.bfloat16)
    update = jnp.dot(basis, ratio, preferred_element_type=jnp.float32)
    by_head = update.reshape(D, HEADS, HD)
    head_mean = lax.optimization_barrier(jnp.mean(by_head * by_head, axis=(0, 2)))
    head_scale = 1.0 / jnp.sqrt(head_mean + norm_floor)
    step = (by_head * head_scale[None, :, None]).reshape(D, HEADS * HD)
    weight = master - step_rate * step
    return (step, weight, weight.astype(jnp.bfloat16), first_new, second_new)

def reference(saved_input, query_cot, key_cot, query_master, key_master, query_basis, key_basis, query_first, query_second, key_first, key_second):
    query_out = update_one(saved_input, query_cot, query_master, query_basis, query_first, query_second)
    key_out = update_one(saved_input, key_cot, key_master, key_basis, key_first, key_second)
    return (query_out[0], query_out[1], query_out[2], query_out[3], query_out[4], key_out[0], key_out[1], key_out[2], key_out[3], key_out[4])
```

```python
import functools

import jax
import jax.numpy as jnp
from jax import lax
from jax.experimental import pallas as pl
from jax.experimental.pallas import tpu as pltpu
from jax.sharding import PartitionSpec as P

HD = 128

moment_decay = 0.8
square_decay = 0.9
square_floor = 1.0
norm_floor = 0.01
step_rate = 0.01

BF = jnp.bfloat16
F32 = jnp.float32
MESH = pl.DeviceIdType.MESH


def exchange_kernel(
    fs,
    tp,
    x_hbm,
    qc_hbm,
    kc_hbm,
    qm_hbm,
    km_hbm,
    qb_hbm,
    kb_hbm,
    qf_ref,
    qs_ref,
    kf_ref,
    ks_ref,
    qfn_ref,
    qsn_ref,
    kfn_ref,
    ksn_ref,
    ratio_ref,
    sums_ref,
    gathered,
    basis_out,
    basis,
    x_v,
    cot,
    master,
    rounded,
    half_send,
    half_recv,
    half_own,
    z_send,
    z_recv,
    low,
    proj,
    proj_send,
    proj_recv,
    load_sem,
    b_send,
    b_recv,
    d_send,
    d_recv,
    p_send,
    p_recv,
    zr_send,
    zr_recv,
    zg_send,
    zg_recv,
    pf_send,
    pf_recv,
    rs_send,
    rs_recv,
    ag_send,
    ag_recv,
    m_send,
    m_recv,
    out_sem,
):
    f = lax.axis_index("fs")
    t = lax.axis_index("tp")
    z, c = t // 2, t % 2
    depth = tp // 2
    relay = fs == 4
    rows, rank = qb_hbm.shape
    width = qc_hbm.shape[1]
    tokens, columns = x_v.shape
    part = rank // fs
    half_rows = rows // 2
    half = tokens // 2
    chunk = tokens // tp

    def at(start, size):
        return pl.ds(pl.multiple_of(start, size), size)

    def remote(src, dst, send, recv, df, dt):
        return pltpu.make_async_remote_copy(
            src_ref=src,
            dst_ref=dst,
            send_sem=send,
            recv_sem=recv,
            device_id=(df, dt),
            device_id_type=MESH,
        )

    loads = [
        pltpu.make_async_copy(qb_hbm, basis.at[0, at(f * rows, rows)], load_sem.at[0]),
        pltpu.make_async_copy(kb_hbm, basis.at[1, at(f * rows, rows)], load_sem.at[1]),
        pltpu.make_async_copy(qm_hbm, master.at[0], load_sem.at[2]),
        pltpu.make_async_copy(km_hbm, master.at[1], load_sem.at[3]),
        pltpu.make_async_copy(x_hbm, x_v, load_sem.at[4]),
        pltpu.make_async_copy(qc_hbm, cot.at[0], load_sem.at[5]),
        pltpu.make_async_copy(kc_hbm, cot.at[1], load_sem.at[6]),
    ]
    for load in loads:
        load.start()

    barrier = pltpu.get_barrier_semaphore()
    for m in range(1, fs):
        pl.semaphore_signal(barrier, inc=1, device_id=(f ^ m, t), device_id_type=MESH)
    pl.semaphore_signal(barrier, inc=1, device_id=(f, t ^ 1), device_id_type=MESH)
    for d in range(1, depth):
        other = lax.rem(z + d, depth) * 2 + c
        pl.semaphore_signal(barrier, inc=1, device_id=(f, other), device_id_type=MESH)
    loads[0].wait()
    loads[1].wait()
    pl.semaphore_wait(barrier, fs - 1 + depth)

    def basis_copy(j, m, owner, target):
        piece = basis.at[j, at(owner * rows + c * half_rows, half_rows)]
        return remote(piece, piece, b_send.at[m, j], b_recv.at[m, j], target, t)

    direct = [m for m in range(1, fs) if not (relay and m == 3)]
    basis_copies = {}
    for m in direct:
        for j in (0, 1) if m % 2 else (1, 0):
            basis_copies[m, j] = basis_copy(j, m, f, f ^ m)
            basis_copies[m, j].start()

    loads[2].wait()
    loads[3].wait()
    tile = min(rows, 128)

    for j in range(2):

        @pl.loop(0, rows // tile)
        def _(i, j=j):
            place = at(i * tile, tile)
            rounded[j, place, :] = master[j, place, :].astype(BF)

    def master_copy(j, m):
        return remote(
            rounded.at[j],
            gathered.at[j, at(f * rows, rows)],
            m_send.at[m, j],
            m_recv.at[m, j],
            f ^ m,
            t,
        )

    def master_relay(j, source, target):
        piece = gathered.at[j, at((f ^ source) * rows, rows)]
        return remote(piece, piece, m_send.at[3, j], m_recv.at[3, j], f ^ target, t)

    if relay:
        basis_copies[1, 0].wait_recv()
        basis_copies[3, 0] = basis_copy(0, 3, f ^ 1, f ^ 2)
        basis_copies[3, 0].start()
        basis_copies[2, 1].wait_recv()
        basis_copies[3, 1] = basis_copy(1, 3, f ^ 2, f ^ 1)
        basis_copies[3, 1].start()

    master_copies = {}
    first_masters = [(1, 0), (2, 1)] if relay else [(m, 0) for m in direct]
    for m, j in first_masters:
        master_copies[m, j] = master_copy(j, m)
        master_copies[m, j].start()

    waited = {(1, 0), (2, 1)} if relay else set()
    for m in range(1, fs):
        for j in range(2):
            if (m, j) not in waited:
                basis_copies[m, j].wait_recv()

    partner_copies = []
    for m in range(1, fs):
        piece = basis.at[:, at((f ^ m) * rows + c * half_rows, half_rows)]
        copy = remote(piece, piece, d_send.at[m], d_recv.at[m], f, t ^ 1)
        copy.start()
        partner_copies.append(copy)

    loads[4].wait()
    step = min(half, 256)

    def project(start, j):
        return jnp.dot(
            x_v[at(start, step), :],
            basis[j, at(t * columns, columns), :],
            preferred_element_type=F32,
        )

    for j in range(2):

        @pl.loop(0, half // step)
        def _(i, j=j):
            half_send[at(i * step, step), j * rank : (j + 1) * rank] = project(
                (1 - c) * half + i * step, j
            ).astype(BF)

    swap = remote(half_send, half_recv, p_send, p_recv, f, t ^ 1)
    swap.start()
    for j in range(2):

        @pl.loop(0, half // step)
        def _(i, j=j):
            half_own[at(i * step, step), j * rank : (j + 1) * rank] = project(
                c * half + i * step, j
            )

    swap.wait_recv()

    @pl.loop(0, half // chunk)
    def _(i):
        place = at(i * chunk, chunk)
        both = half_own[place, :] + half_recv[place, :].astype(F32)
        half_own[place, :] = both
        z_send[place, :] = both.astype(BF)

    z_copies = []
    for d in range(1, depth):
        other = lax.rem(z + d, depth)
        copy = remote(
            z_send.at[at(other * chunk, chunk)],
            z_recv.at[d],
            zr_send.at[d],
            zr_recv.at[d],
            f,
            other * 2 + c,
        )
        copy.start()
        z_copies.append(copy)
    total = half_own[at(z * chunk, chunk), :]
    for d in range(1, depth):
        z_copies[d - 1].wait_recv()
        total = total + z_recv[d].astype(F32)
    low[at(c * half + z * chunk, chunk), :] = total.astype(BF)

    def low_piece(d, core):
        return low.at[at(core * half + lax.rem(z + depth - d, depth) * chunk, chunk)]

    g_copies = []
    for d in range(1, depth):
        other = lax.rem(z + d, depth)
        copy = remote(
            low_piece(0, c), low_piece(0, c), zg_send.at[d], zg_recv.at[d], f, other * 2 + c
        )
        copy.start()
        g_copies.append(copy)
    forwards = []
    for d in range(depth):
        if d > 0:
            g_copies[d - 1].wait_recv()
        copy = remote(low_piece(d, c), low_piece(d, c), pf_send.at[d], pf_recv.at[d], f, t ^ 1)
        copy.start()
        forwards.append(copy)
    loads[5].wait()
    loads[6].wait()
    for copy in forwards:
        copy.wait_recv()

    for j in range(2):
        product = lax.dot_general(
            low[:, j * rank : (j + 1) * rank],
            cot[j],
            (((0,), (0,)), ((), ())),
            preferred_element_type=F32,
        )
        proj[j] = product
        proj_send[j] = product.astype(BF)
    r_copies = []
    for m in range(1, fs):
        copy = remote(
            proj_send.at[:, at((f ^ m) * part, part)],
            proj_recv.at[m],
            rs_send.at[m],
            rs_recv.at[m],
            f ^ m,
            t,
        )
        copy.start()
        r_copies.append(copy)
    for copy in r_copies:
        copy.wait_recv()

    own = at(f * part, part)
    moments = ((qf_ref, qs_ref, qfn_ref, qsn_ref), (kf_ref, ks_ref, kfn_ref, ksn_ref))
    for j, (first, second, first_out, second_out) in enumerate(moments):
        summed = proj[j, own, :]
        for m in range(1, fs):
            summed = summed + proj_recv[m, j].astype(F32)
        first_new = moment_decay * first[...] + (1.0 - moment_decay) * summed
        second_new = square_decay * second[...] + (1.0 - square_decay) * summed * summed
        first_out[...] = first_new
        second_out[...] = second_new
        ratio_ref[j, own, :] = (first_new / jnp.sqrt(second_new + square_floor)).astype(BF)

    a_copies = []
    for m in range(1, fs):
        piece = ratio_ref.at[:, own]
        copy = remote(piece, piece, ag_send.at[m], ag_recv.at[m], f ^ m, t)
        copy.start()
        a_copies.append(copy)

    for m in direct:
        for j in range(2):
            if (m, j) not in master_copies:
                master_copies[m, j] = master_copy(j, m)
                master_copies[m, j].start()
    if relay:
        master_copies[1, 0].wait_recv()
        master_copies[3, 0] = master_relay(0, 1, 2)
        master_copies[3, 0].start()
        master_copies[2, 1].wait_recv()
        master_copies[3, 1] = master_relay(1, 2, 1)
        master_copies[3, 1].start()

    for copy in partner_copies:
        copy.wait_recv()
    store = pltpu.make_async_copy(basis, basis_out, out_sem)
    store.start()
    for copy in a_copies:
        copy.wait_recv()

    high = min(rows, 256)
    for j in range(2):

        def add(i, total, j=j):
            update = jnp.dot(
                basis[j, at(i * high, high), :], ratio_ref[j], preferred_element_type=F32
            )
            return total + jnp.sum((update * update).reshape(high // 8, 8, width), axis=0)

        sums_ref[j] = lax.fori_loop(0, fs * rows // high, add, jnp.zeros((8, width), F32))

    store.wait()
    early = {(1, 0), (2, 1)} if relay else set()
    for m in range(1, fs):
        for j in range(2):
            if (m, j) not in early:
                master_copies[m, j].wait_recv()
    for copy in list(basis_copies.values()) + partner_copies + [swap] + z_copies:
        copy.wait_send()
    for copy in g_copies + forwards + r_copies + a_copies + list(master_copies.values()):
        copy.wait_send()


def final_kernel(
    own_steps,
    fs_ref,
    sums_ref,
    ratio_ref,
    basis_ref,
    gathered_ref,
    qm_ref,
    km_ref,
    qstep_ref,
    qweight_ref,
    qcopy_ref,
    kstep_ref,
    kweight_ref,
    kcopy_ref,
    *,
    count,
):
    i = pl.program_id(0)
    outs = ((qm_ref, qstep_ref, qweight_ref, qcopy_ref), (km_ref, kstep_ref, kweight_ref, kcopy_ref))
    for j, (master, step_out, weight_out, copy_out) in enumerate(outs):
        sums = jnp.sum(sums_ref[j], axis=0, keepdims=True)
        heads = []
        for h in range(sums.shape[1] // HD):
            total = jnp.sum(sums[:, h * HD : (h + 1) * HD], axis=1, keepdims=True)
            scale = 1.0 / jnp.sqrt(total / (count * HD) + norm_floor)
            heads.append(jnp.broadcast_to(scale, (1, HD)))
        scale = jnp.concatenate(heads, axis=1)
        update = jnp.dot(basis_ref[j], ratio_ref[j], preferred_element_type=F32)
        step = update * scale

        @pl.when(i < own_steps)
        def _(master=master, step_out=step_out, weight_out=weight_out, copy_out=copy_out, step=step):
            weight = master[...] - step_rate * step
            step_out[...] = step
            weight_out[...] = weight
            copy_out[...] = weight.astype(BF)

        @pl.when(i >= own_steps)
        def _(j=j, copy_out=copy_out, step=step):
            copy_out[...] = (gathered_ref[j].astype(F32) - step_rate * step).astype(BF)


def body(fs, tp, *args):
    saved_input, query_cot, _, query_master, key_master, query_basis = args[:6]
    rows, rank = query_basis.shape
    tokens, columns = saved_input.shape
    width = query_cot.shape[1]
    part = rank // fs
    depth = tp // 2
    count = fs * rows
    half, chunk = tokens // 2, tokens // tp
    any_spec = pl.BlockSpec(memory_space=pl.ANY)
    vmem = pl.BlockSpec(memory_space=pltpu.VMEM)
    dma = pltpu.SemaphoreType.DMA
    moment = jax.ShapeDtypeStruct((part, width), F32)
    pairs = []
    for shape in ((fs, 2), (fs,), (), (depth,), (depth,), (depth,), (fs,), (fs,), (fs, 2)):
        pairs += [dma(shape), dma(shape)]
    results = pl.pallas_call(
        functools.partial(exchange_kernel, fs, tp),
        name="exchange",
        out_shape=(
            moment,
            moment,
            moment,
            moment,
            jax.ShapeDtypeStruct((2, rank, width), BF),
            jax.ShapeDtypeStruct((2, 8, width), F32),
            jax.ShapeDtypeStruct((2, count, width), BF),
            jax.ShapeDtypeStruct((2, count, rank), BF),
        ),
        in_specs=[any_spec] * 7 + [vmem] * 4,
        out_specs=(vmem,) * 6 + (any_spec,) * 2,
        scratch_shapes=[
            pltpu.VMEM((2, count, rank), BF),
            pltpu.VMEM((tokens, columns), BF),
            pltpu.VMEM((2, tokens, width), BF),
            pltpu.VMEM((2, rows, width), F32),
            pltpu.VMEM((2, rows, width), BF),
            pltpu.VMEM((half, 2 * rank), BF),
            pltpu.VMEM((half, 2 * rank), BF),
            pltpu.VMEM((half, 2 * rank), F32),
            pltpu.VMEM((half, 2 * rank), BF),
            pltpu.VMEM((depth, chunk, 2 * rank), BF),
            pltpu.VMEM((tokens, 2 * rank), BF),
            pltpu.VMEM((2, rank, width), F32),
            pltpu.VMEM((2, rank, width), BF),
            pltpu.VMEM((fs, 2, part, width), BF),
            dma((7,)),
            *pairs,
            dma,
        ],
        compiler_params=pltpu.CompilerParams(
            collective_id=0, has_side_effects=True, vmem_limit_bytes=60 * 1024 * 1024
        ),
    )(*args)
    qfn, qsn, kfn, ksn, ratio, sums, gathered, basis = results

    tile = min(rows, 256)
    own_steps = rows // tile
    steps = count // tile

    def own_row(i, place):
        return (jnp.minimum(i, own_steps - 1), 0)

    def full_row(i, place):
        return (lax.rem(place[0] * own_steps + i, steps), 0)

    def full_pair(i, place):
        return (0, lax.rem(place[0] * own_steps + i, steps), 0)

    def gathered_pair(i, place):
        return (0, lax.rem(place[0] * own_steps + jnp.maximum(i, own_steps), steps), 0)

    def whole(i, place):
        return (0, 0, 0)

    own_spec = pl.BlockSpec((tile, width), own_row)
    full_spec = pl.BlockSpec((tile, width), full_row)
    place = jnp.reshape(lax.axis_index("fs"), (1,)).astype(jnp.int32)
    big = jax.ShapeDtypeStruct((rows, width), F32)
    copied = jax.ShapeDtypeStruct((count, width), BF)
    qstep, qweight, qcopy, kstep, kweight, kcopy = pl.pallas_call(
        functools.partial(final_kernel, own_steps, count=count),
        name="final",
        out_shape=(big, big, copied, big, big, copied),
        grid_spec=pltpu.PrefetchScalarGridSpec(
            num_scalar_prefetch=1,
            grid=(steps,),
            in_specs=[
                pl.BlockSpec((2, 8, width), whole),
                pl.BlockSpec((2, rank, width), whole),
                pl.BlockSpec((2, tile, rank), full_pair),
                pl.BlockSpec((2, tile, width), gathered_pair),
                own_spec,
                own_spec,
            ],
            out_specs=(own_spec, own_spec, full_spec, own_spec, own_spec, full_spec),
        ),
        compiler_params=pltpu.CompilerParams(vmem_limit_bytes=48 * 1024 * 1024),
    )(place, sums, ratio, basis, gathered, query_master, key_master)
    return (qstep, qweight, qcopy, qfn, qsn, kstep, kweight, kcopy, kfn, ksn)


def solution(mesh):
    split, tall, wide = P("fs", "tp"), P("fs", None), P(None, "tp")
    outs = (split, split, wide, split, split)
    return jax.shard_map(
        functools.partial(body, mesh.shape["fs"], mesh.shape["tp"]),
        mesh=mesh,
        in_specs=(split,) * 5 + (tall, tall) + (split,) * 4,
        out_specs=outs + outs,
        check_vma=False,
    )
```

```python
import functools

import jax
import jax.numpy as jnp
from jax import lax
from jax.experimental import pallas as pl
from jax.experimental.pallas import tpu as pltpu
from jax.sharding import PartitionSpec as P

HD = 128

moment_decay = 0.8
square_decay = 0.9
square_floor = 1.0
norm_floor = 0.01
step_rate = 0.01

BF = jnp.bfloat16
F32 = jnp.float32
MESH = pl.DeviceIdType.MESH


def exchange_kernel(
    fs,
    tp,
    x_hbm,
    qc_hbm,
    kc_hbm,
    qm_hbm,
    km_hbm,
    qb_hbm,
    kb_hbm,
    qf_ref,
    qs_ref,
    kf_ref,
    ks_ref,
    qfn_ref,
    qsn_ref,
    kfn_ref,
    ksn_ref,
    ratio_ref,
    scale_ref,
    gathered,
    basis_out,
    basis,
    x_v,
    cot,
    master,
    rounded,
    half_send,
    half_recv,
    half_own,
    z_send,
    z_recv,
    low,
    proj,
    proj_send,
    proj_recv,
    load_sem,
    b_send,
    b_recv,
    d_send,
    d_recv,
    p_send,
    p_recv,
    zr_send,
    zr_recv,
    zg_send,
    zg_recv,
    pf_send,
    pf_recv,
    rs_send,
    rs_recv,
    ag_send,
    ag_recv,
    m_send,
    m_recv,
    out_sem,
):
    f = lax.axis_index("fs")
    t = lax.axis_index("tp")
    z, c = t // 2, t % 2
    depth = tp // 2
    relay = fs == 4
    rows, rank = qb_hbm.shape
    width = qc_hbm.shape[1]
    tokens, columns = x_v.shape
    part = rank // fs
    half_rows = rows // 2
    half = tokens // 2
    chunk = tokens // tp

    def at(start, size):
        return pl.ds(pl.multiple_of(start, size), size)

    def remote(src, dst, send, recv, df, dt):
        return pltpu.make_async_remote_copy(
            src_ref=src,
            dst_ref=dst,
            send_sem=send,
            recv_sem=recv,
            device_id=(df, dt),
            device_id_type=MESH,
        )

    loads = [
        pltpu.make_async_copy(qb_hbm, basis.at[0, at(f * rows, rows)], load_sem.at[0]),
        pltpu.make_async_copy(kb_hbm, basis.at[1, at(f * rows, rows)], load_sem.at[1]),
        pltpu.make_async_copy(qm_hbm, master.at[0], load_sem.at[2]),
        pltpu.make_async_copy(km_hbm, master.at[1], load_sem.at[3]),
        pltpu.make_async_copy(x_hbm, x_v, load_sem.at[4]),
        pltpu.make_async_copy(qc_hbm, cot.at[0], load_sem.at[5]),
        pltpu.make_async_copy(kc_hbm, cot.at[1], load_sem.at[6]),
    ]
    for load in loads:
        load.start()

    barrier = pltpu.get_barrier_semaphore()
    for m in range(1, fs):
        pl.semaphore_signal(barrier, inc=1, device_id=(f ^ m, t), device_id_type=MESH)
    pl.semaphore_signal(barrier, inc=1, device_id=(f, t ^ 1), device_id_type=MESH)
    for d in range(1, depth):
        other = lax.rem(z + d, depth) * 2 + c
        pl.semaphore_signal(barrier, inc=1, device_id=(f, other), device_id_type=MESH)
    loads[0].wait()
    loads[1].wait()
    pl.semaphore_wait(barrier, fs - 1 + depth)

    def basis_copy(j, m, owner, target):
        piece = basis.at[j, at(owner * rows + c * half_rows, half_rows)]
        return remote(piece, piece, b_send.at[m, j], b_recv.at[m, j], target, t)

    direct = [m for m in range(1, fs) if not (relay and m == 3)]
    basis_copies = {}
    for m in direct:
        for j in (0, 1) if m % 2 else (1, 0):
            basis_copies[m, j] = basis_copy(j, m, f, f ^ m)
            basis_copies[m, j].start()

    loads[2].wait()
    loads[3].wait()
    tile = min(rows, 128)

    for j in range(2):

        @pl.loop(0, rows // tile)
        def _(i, j=j):
            place = at(i * tile, tile)
            rounded[j, place, :] = master[j, place, :].astype(BF)

    def master_copy(j, m):
        return remote(
            rounded.at[j],
            gathered.at[j, at(f * rows, rows)],
            m_send.at[m, j],
            m_recv.at[m, j],
            f ^ m,
            t,
        )

    def master_relay(j, side):
        source = 1 + j
        piece = gathered.at[j, at((f ^ source) * rows + side * half_rows, half_rows)]
        slot = 3 + side
        return remote(piece, piece, m_send.at[slot, j], m_recv.at[slot, j], f ^ (2 - j), t)

    if relay:
        basis_copies[1, 0].wait_recv()
        basis_copies[3, 0] = basis_copy(0, 3, f ^ 1, f ^ 2)
        basis_copies[3, 0].start()
        basis_copies[2, 1].wait_recv()
        basis_copies[3, 1] = basis_copy(1, 3, f ^ 2, f ^ 1)
        basis_copies[3, 1].start()

    master_copies = {}
    for turn in range(2):
        for m in direct:
            j = (m + 1 + turn) % 2
            master_copies[m, j] = master_copy(j, m)
            master_copies[m, j].start()
    kept = pltpu.make_async_copy(rounded, gathered.at[:, at(f * rows, rows)], out_sem.at[1])
    kept.start()

    waited = {(1, 0), (2, 1)} if relay else set()
    for m in range(1, fs):
        for j in range(2):
            if (m, j) not in waited:
                basis_copies[m, j].wait_recv()

    loads[4].wait()
    step = min(half, 256)

    def project(start, j):
        return jnp.dot(
            x_v[at(start, step), :],
            basis[j, at(t * columns, columns), :],
            preferred_element_type=F32,
        )

    for j in range(2):

        @pl.loop(0, half // step)
        def _(i, j=j):
            half_send[at(i * step, step), j * rank : (j + 1) * rank] = project(
                (1 - c) * half + i * step, j
            ).astype(BF)

    swap = remote(half_send, half_recv, p_send, p_recv, f, t ^ 1)
    swap.start()
    for j in range(2):

        @pl.loop(0, half // step)
        def _(i, j=j):
            half_own[at(i * step, step), j * rank : (j + 1) * rank] = project(
                c * half + i * step, j
            )

    swap.wait_recv()

    partner_copies = []
    for m in range(1, fs):
        piece = basis.at[:, at((f ^ m) * rows + c * half_rows, half_rows)]
        copy = remote(piece, piece, d_send.at[m], d_recv.at[m], f, t ^ 1)
        copy.start()
        partner_copies.append(copy)

    @pl.loop(0, half // chunk)
    def _(i):
        place = at(i * chunk, chunk)
        both = half_own[place, :] + half_recv[place, :].astype(F32)
        half_own[place, :] = both
        z_send[place, :] = both.astype(BF)

    z_copies = []
    for d in range(1, depth):
        other = lax.rem(z + d, depth)
        copy = remote(
            z_send.at[at(other * chunk, chunk)],
            z_recv.at[d],
            zr_send.at[d],
            zr_recv.at[d],
            f,
            other * 2 + c,
        )
        copy.start()
        z_copies.append(copy)
    total = half_own[at(z * chunk, chunk), :]
    for d in range(1, depth):
        z_copies[d - 1].wait_recv()
        total = total + z_recv[d].astype(F32)
    low[at(c * half + z * chunk, chunk), :] = total.astype(BF)

    def low_piece(d, core):
        return low.at[at(core * half + lax.rem(z + depth - d, depth) * chunk, chunk)]

    g_copies = []
    for d in range(1, depth):
        other = lax.rem(z + d, depth)
        copy = remote(
            low_piece(0, c), low_piece(0, c), zg_send.at[d], zg_recv.at[d], f, other * 2 + c
        )
        copy.start()
        g_copies.append(copy)
    forwards = []
    for d in range(depth):
        if d > 0:
            g_copies[d - 1].wait_recv()
        copy = remote(low_piece(d, c), low_piece(d, c), pf_send.at[d], pf_recv.at[d], f, t ^ 1)
        copy.start()
        forwards.append(copy)
    loads[5].wait()
    loads[6].wait()
    for copy in forwards:
        copy.wait_recv()

    for j in range(2):
        product = lax.dot_general(
            low[:, j * rank : (j + 1) * rank],
            cot[j],
            (((0,), (0,)), ((), ())),
            preferred_element_type=F32,
        )
        proj[j] = product
        proj_send[j] = product.astype(BF)
    r_copies = []
    for m in range(1, fs):
        copy = remote(
            proj_send.at[:, at((f ^ m) * part, part)],
            proj_recv.at[m],
            rs_send.at[m],
            rs_recv.at[m],
            f ^ m,
            t,
        )
        copy.start()
        r_copies.append(copy)
    if relay:
        for j in range(2):
            master_copies[1 + j, j].wait_recv()
            master_copies[3, j] = master_relay(j, 0)
            master_copies[3, j].start()
    for copy in r_copies:
        copy.wait_recv()

    own = at(f * part, part)
    moments = ((qf_ref, qs_ref, qfn_ref, qsn_ref), (kf_ref, ks_ref, kfn_ref, ksn_ref))
    for j, (first, second, first_out, second_out) in enumerate(moments):
        summed = proj[j, own, :]
        for m in range(1, fs):
            summed = summed + proj_recv[m, j].astype(F32)
        first_new = moment_decay * first[...] + (1.0 - moment_decay) * summed
        second_new = square_decay * second[...] + (1.0 - square_decay) * summed * summed
        first_out[...] = first_new
        second_out[...] = second_new
        ratio_ref[j, own, :] = (first_new / jnp.sqrt(second_new + square_floor)).astype(BF)

    a_copies = []
    for m in range(1, fs):
        piece = ratio_ref.at[:, own]
        copy = remote(piece, piece, ag_send.at[m], ag_recv.at[m], f ^ m, t)
        copy.start()
        a_copies.append(copy)

    if relay:
        for j in range(2):
            master_copies[4, j] = master_relay(j, 1)
            master_copies[4, j].start()

    for copy in partner_copies:
        copy.wait_recv()
    store = pltpu.make_async_copy(basis, basis_out, out_sem.at[0])
    store.start()
    for copy in a_copies:
        copy.wait_recv()

    high = min(rows, 256)
    for j in range(2):

        def add(i, total, j=j):
            update = jnp.dot(
                basis[j, at(i * high, high), :], ratio_ref[j], preferred_element_type=F32
            )
            return total + jnp.sum((update * update).reshape(high // 8, 8, width), axis=0)

        sums = lax.fori_loop(0, fs * rows // high, add, jnp.zeros((8, width), F32))
        sums = jnp.sum(sums, axis=0, keepdims=True)
        for h in range(width // HD):
            head = slice(h * HD, (h + 1) * HD)
            total = jnp.sum(sums[:, head], axis=1, keepdims=True)
            scale = 1.0 / jnp.sqrt(total / (fs * rows * HD) + norm_floor)
            scale_ref[j, :, head] = jnp.broadcast_to(scale, (8, HD))

    store.wait()
    kept.wait()
    early = {(1, 0), (2, 1)} if relay else set()
    for place, copy in master_copies.items():
        if place not in early:
            copy.wait_recv()
    for copy in list(basis_copies.values()) + partner_copies + [swap] + z_copies:
        copy.wait_send()
    for copy in g_copies + forwards + r_copies + a_copies + list(master_copies.values()):
        copy.wait_send()


def final_kernel(*refs):
    scale_ref, ratio_ref, basis_ref, gathered_ref = refs[:4]
    inputs, moments, outs, moments_out = refs[4:8], refs[8:12], refs[12:18], refs[18:]
    for j in range(2):
        scale = scale_ref[j, 0:1, :]
        own_basis, master = inputs[2 * j : 2 * j + 2]
        step_out, weight_out, copy_out = outs[3 * j : 3 * j + 3]
        update = jnp.dot(own_basis[...], ratio_ref[j], preferred_element_type=F32)
        step = update * scale
        step_out[...] = step
        weight_out[...] = master[...] - step_rate * step
        update = jnp.dot(basis_ref[j], ratio_ref[j], preferred_element_type=F32)
        step = update * scale
        copy_out[...] = (gathered_ref[j].astype(F32) - step_rate * step).astype(BF)

    @pl.when(pl.program_id(0) == 0)
    def _():
        for source, target in zip(moments, moments_out):
            target[...] = source[...]


def body(fs, tp, *args):
    saved_input, query_cot, _, query_master, key_master, query_basis, key_basis = args[:7]
    rows, rank = query_basis.shape
    tokens, columns = saved_input.shape
    width = query_cot.shape[1]
    part = rank // fs
    depth = tp // 2
    count = fs * rows
    half, chunk = tokens // 2, tokens // tp
    any_spec = pl.BlockSpec(memory_space=pl.ANY)
    vmem = pl.BlockSpec(memory_space=pltpu.VMEM)
    dma = pltpu.SemaphoreType.DMA
    moment = jax.ShapeDtypeStruct((part, width), F32)
    pairs = []
    for shape in ((fs, 2), (fs,), (), (depth,), (depth,), (depth,), (fs,), (fs,), (fs + 1, 2)):
        pairs += [dma(shape), dma(shape)]
    results = pl.pallas_call(
        functools.partial(exchange_kernel, fs, tp),
        name="exchange",
        out_shape=(
            moment,
            moment,
            moment,
            moment,
            jax.ShapeDtypeStruct((2, rank, width), BF),
            jax.ShapeDtypeStruct((2, 8, width), F32),
            jax.ShapeDtypeStruct((2, count, width), BF),
            jax.ShapeDtypeStruct((2, count, rank), BF),
        ),
        in_specs=[any_spec] * 7 + [vmem] * 4,
        out_specs=(vmem,) * 6 + (any_spec,) * 2,
        scratch_shapes=[
            pltpu.VMEM((2, count, rank), BF),
            pltpu.VMEM((tokens, columns), BF),
            pltpu.VMEM((2, tokens, width), BF),
            pltpu.VMEM((2, rows, width), F32),
            pltpu.VMEM((2, rows, width), BF),
            pltpu.VMEM((half, 2 * rank), BF),
            pltpu.VMEM((half, 2 * rank), BF),
            pltpu.VMEM((half, 2 * rank), F32),
            pltpu.VMEM((half, 2 * rank), BF),
            pltpu.VMEM((depth, chunk, 2 * rank), BF),
            pltpu.VMEM((tokens, 2 * rank), BF),
            pltpu.VMEM((2, rank, width), F32),
            pltpu.VMEM((2, rank, width), BF),
            pltpu.VMEM((fs, 2, part, width), BF),
            dma((7,)),
            *pairs,
            dma((2,)),
        ],
        compiler_params=pltpu.CompilerParams(
            collective_id=0, has_side_effects=True, vmem_limit_bytes=60 * 1024 * 1024
        ),
    )(*args)
    moments, (ratio, scale, gathered, basis) = results[:4], results[4:]

    steps = min(8, rows // 16)
    own_tile, tile = rows // steps, count // steps

    def row(i):
        return (i, 0)

    def pair(i):
        return (0, i, 0)

    def whole(i):
        return (0, 0, 0)

    own_spec = pl.BlockSpec((own_tile, width), row)
    full_spec = pl.BlockSpec((tile, width), row)
    basis_spec = pl.BlockSpec((own_tile, rank), row)
    moment_spec = pl.BlockSpec((part, width), lambda i: (0, 0))
    big = jax.ShapeDtypeStruct((rows, width), F32)
    copied = jax.ShapeDtypeStruct((count, width), BF)
    outs = pl.pallas_call(
        final_kernel,
        name="final",
        out_shape=(big, big, copied) * 2 + (moment,) * 4,
        grid=(steps,),
        in_specs=[
            pl.BlockSpec((2, 8, width), whole),
            pl.BlockSpec((2, rank, width), whole),
            pl.BlockSpec((2, tile, rank), pair),
            pl.BlockSpec((2, tile, width), pair),
            basis_spec,
            own_spec,
            basis_spec,
            own_spec,
        ]
        + [moment_spec] * 4,
        out_specs=(own_spec, own_spec, full_spec) * 2 + (moment_spec,) * 4,
        compiler_params=pltpu.CompilerParams(vmem_limit_bytes=60 * 1024 * 1024),
    )(scale, ratio, basis, gathered, query_basis, query_master, key_basis, key_master, *moments)
    return (*outs[:3], *outs[6:8], *outs[3:6], *outs[8:])


def solution(mesh):
    split, tall, wide = P("fs", "tp"), P("fs", None), P(None, "tp")
    outs = (split, split, wide, split, split)
    return jax.shard_map(
        functools.partial(body, mesh.shape["fs"], mesh.shape["tp"]),
        mesh=mesh,
        in_specs=(split,) * 5 + (tall, tall) + (split,) * 4,
        out_specs=outs + outs,
        check_vma=False,
    )
```

```python
import functools

import jax
import jax.numpy as jnp
from jax import lax
from jax.experimental import pallas as pl
from jax.experimental.pallas import tpu as pltpu
from jax.sharding import PartitionSpec as P

HD = 128

moment_decay = 0.8
square_decay = 0.9
square_floor = 1.0
norm_floor = 0.01
step_rate = 0.01

BF = jnp.bfloat16
F32 = jnp.float32
MESH = pl.DeviceIdType.MESH


def exchange_kernel(
    fs,
    tp,
    x_hbm,
    qc_hbm,
    kc_hbm,
    qm_hbm,
    km_hbm,
    qb_hbm,
    kb_hbm,
    qf_ref,
    qs_ref,
    kf_ref,
    ks_ref,
    qfn_ref,
    qsn_ref,
    kfn_ref,
    ksn_ref,
    ratio_ref,
    scale_ref,
    gathered,
    basis_out,
    basis,
    x_v,
    cot,
    master,
    rounded,
    half_send,
    half_recv,
    half_own,
    z_send,
    z_recv,
    low,
    proj,
    proj_send,
    proj_recv,
    load_sem,
    b_send,
    b_recv,
    d_send,
    d_recv,
    zb_send,
    zb_recv,
    p_send,
    p_recv,
    zr_send,
    zr_recv,
    zg_send,
    zg_recv,
    pf_send,
    pf_recv,
    rs_send,
    rs_recv,
    ag_send,
    ag_recv,
    m_send,
    m_recv,
    out_sem,
):
    f = lax.axis_index("fs")
    t = lax.axis_index("tp")
    z, c = t // 2, t % 2
    depth = tp // 2
    relay = fs == 4
    rows, rank = qb_hbm.shape
    width = qc_hbm.shape[1]
    tokens, columns = x_v.shape
    part = rank // fs
    half_rows = rows // 2
    half = tokens // 2
    chunk = tokens // tp

    def at(start, size):
        return pl.ds(pl.multiple_of(start, size), size)

    def remote(src, dst, send, recv, df, dt):
        return pltpu.make_async_remote_copy(
            src_ref=src,
            dst_ref=dst,
            send_sem=send,
            recv_sem=recv,
            device_id=(df, dt),
            device_id_type=MESH,
        )

    loads = [
        pltpu.make_async_copy(qb_hbm, basis.at[0, at(f * rows, rows)], load_sem.at[0]),
        pltpu.make_async_copy(kb_hbm, basis.at[1, at(f * rows, rows)], load_sem.at[1]),
        pltpu.make_async_copy(qm_hbm, master.at[0], load_sem.at[2]),
        pltpu.make_async_copy(km_hbm, master.at[1], load_sem.at[3]),
        pltpu.make_async_copy(x_hbm, x_v, load_sem.at[4]),
        pltpu.make_async_copy(qc_hbm, cot.at[0], load_sem.at[5]),
        pltpu.make_async_copy(kc_hbm, cot.at[1], load_sem.at[6]),
    ]
    for load in loads:
        load.start()

    barrier = pltpu.get_barrier_semaphore()
    for m in range(1, fs):
        pl.semaphore_signal(barrier, inc=1, device_id=(f ^ m, t), device_id_type=MESH)
    pl.semaphore_signal(barrier, inc=1, device_id=(f, t ^ 1), device_id_type=MESH)
    for d in range(1, depth):
        other = lax.rem(z + d, depth) * 2 + c
        pl.semaphore_signal(barrier, inc=1, device_id=(f, other), device_id_type=MESH)
    loads[0].wait()
    loads[1].wait()
    pl.semaphore_wait(barrier, fs - 1 + depth)

    def basis_copy(j, m, owner, target):
        piece = basis.at[j, at(owner * rows + c * half_rows, half_rows)]
        return remote(piece, piece, b_send.at[m, j], b_recv.at[m, j], target, t)

    direct = [m for m in range(1, fs) if not (relay and m == 3)]
    basis_copies = {}
    for m in direct:
        for j in (0, 1) if m % 2 else (1, 0):
            basis_copies[m, j] = basis_copy(j, m, f, f ^ m)
    if relay:
        basis_copies[3, 0] = basis_copy(0, 3, f ^ 1, f ^ 2)
        basis_copies[3, 1] = basis_copy(1, 3, f ^ 2, f ^ 1)

    @pl.when(f == z)
    def _():
        for m in direct:
            for j in (0, 1) if m % 2 else (1, 0):
                basis_copies[m, j].start()

    loads[2].wait()
    loads[3].wait()
    tile = min(rows, 128)

    for j in range(2):

        @pl.loop(0, rows // tile)
        def _(i, j=j):
            place = at(i * tile, tile)
            rounded[j, place, :] = master[j, place, :].astype(BF)

    def master_copy(j, m):
        return remote(
            rounded.at[j],
            gathered.at[j, at(f * rows, rows)],
            m_send.at[m, j],
            m_recv.at[m, j],
            f ^ m,
            t,
        )

    def master_relay(j, side):
        source = 1 + j
        piece = gathered.at[j, at((f ^ source) * rows + side * half_rows, half_rows)]
        slot = 3 + side
        return remote(piece, piece, m_send.at[slot, j], m_recv.at[slot, j], f ^ (2 - j), t)

    if relay:
        for j in range(2):

            @pl.when(f ^ (1 + j) == z)
            def _(j=j):
                basis_copies[1 + j, j].wait_recv()
                basis_copies[3, j].start()

    master_copies = {}
    for turn in range(2):
        for m in direct:
            j = (m + 1 + turn) % 2
            master_copies[m, j] = master_copy(j, m)
            master_copies[m, j].start()
    kept = pltpu.make_async_copy(rounded, gathered.at[:, at(f * rows, rows)], out_sem.at[1])
    kept.start()

    waited = {(1, 0), (2, 1)} if relay else set()
    for m in range(1, fs):

        @pl.when(f ^ m == z)
        def _(m=m):
            for j in range(2):
                if (m, j) not in waited:
                    basis_copies[m, j].wait_recv()

    loads[4].wait()
    step = min(half, 256)

    def project(start, j):
        return jnp.dot(
            x_v[at(start, step), :],
            basis[j, at(t * columns, columns), :],
            preferred_element_type=F32,
        )

    for j in range(2):

        @pl.loop(0, half // step)
        def _(i, j=j):
            half_send[at(i * step, step), j * rank : (j + 1) * rank] = project(
                (1 - c) * half + i * step, j
            ).astype(BF)

    swap = remote(half_send, half_recv, p_send, p_recv, f, t ^ 1)
    swap.start()
    for j in range(2):

        @pl.loop(0, half // step)
        def _(i, j=j):
            half_own[at(i * step, step), j * rank : (j + 1) * rank] = project(
                c * half + i * step, j
            )

    swap.wait_recv()

    @pl.loop(0, half // chunk)
    def _(i):
        place = at(i * chunk, chunk)
        both = half_own[place, :] + half_recv[place, :].astype(F32)
        half_own[place, :] = both
        z_send[place, :] = both.astype(BF)

    z_copies = []
    for d in range(1, depth):
        other = lax.rem(z + d, depth)
        copy = remote(
            z_send.at[at(other * chunk, chunk)],
            z_recv.at[d],
            zr_send.at[d],
            zr_recv.at[d],
            f,
            other * 2 + c,
        )
        copy.start()
        z_copies.append(copy)
    total = half_own[at(z * chunk, chunk), :]
    for d in range(1, depth):
        z_copies[d - 1].wait_recv()
        total = total + z_recv[d].astype(F32)
    low[at(c * half + z * chunk, chunk), :] = total.astype(BF)

    def low_piece(d, core):
        return low.at[at(core * half + lax.rem(z + depth - d, depth) * chunk, chunk)]

    g_copies = []
    for d in range(1, depth):
        other = lax.rem(z + d, depth)
        copy = remote(
            low_piece(0, c), low_piece(0, c), zg_send.at[d], zg_recv.at[d], f, other * 2 + c
        )
        copy.start()
        g_copies.append(copy)

    def block(d):
        return lax.rem(z + depth - d, depth)

    def block_piece(d):
        return basis.at[:, at(block(d) * rows + c * half_rows, half_rows)]

    plane_copies, partner_copies = [], []
    for d in range(depth):
        piece = block_piece(d)
        partner_copies.append(remote(piece, piece, d_send.at[d], d_recv.at[d], f, t ^ 1))
        piece = block_piece(0)
        other = lax.rem(z + d, depth) * 2 + c
        plane_copies.append(remote(piece, piece, zb_send.at[d], zb_recv.at[d], f, other))

    @pl.when(f != z)
    def _():
        for copy in plane_copies[1:]:
            copy.start()

    forwards = []
    for d in range(depth):
        if d > 0:
            g_copies[d - 1].wait_recv()
        copy = remote(low_piece(d, c), low_piece(d, c), pf_send.at[d], pf_recv.at[d], f, t ^ 1)
        copy.start()
        forwards.append(copy)
    loads[5].wait()
    loads[6].wait()
    for copy in forwards:
        copy.wait_recv()

    for j in range(2):
        product = lax.dot_general(
            low[:, j * rank : (j + 1) * rank],
            cot[j],
            (((0,), (0,)), ((), ())),
            preferred_element_type=F32,
        )
        proj[j] = product
        proj_send[j] = product.astype(BF)
    r_copies = []
    for m in range(1, fs):
        copy = remote(
            proj_send.at[:, at((f ^ m) * part, part)],
            proj_recv.at[m],
            rs_send.at[m],
            rs_recv.at[m],
            f ^ m,
            t,
        )
        copy.start()
        r_copies.append(copy)
    if relay:
        for j in range(2):
            master_copies[1 + j, j].wait_recv()
            master_copies[3, j] = master_relay(j, 0)
            master_copies[3, j].start()
    for copy in r_copies:
        copy.wait_recv()

    own = at(f * part, part)
    moments = ((qf_ref, qs_ref, qfn_ref, qsn_ref), (kf_ref, ks_ref, kfn_ref, ksn_ref))
    for j, (first, second, first_out, second_out) in enumerate(moments):
        summed = proj[j, own, :]
        for m in range(1, fs):
            summed = summed + proj_recv[m, j].astype(F32)
        first_new = moment_decay * first[...] + (1.0 - moment_decay) * summed
        second_new = square_decay * second[...] + (1.0 - square_decay) * summed * summed
        first_out[...] = first_new
        second_out[...] = second_new
        ratio_ref[j, own, :] = (first_new / jnp.sqrt(second_new + square_floor)).astype(BF)

    a_copies = []
    for m in range(1, fs):
        piece = ratio_ref.at[:, own]
        copy = remote(piece, piece, ag_send.at[m], ag_recv.at[m], f ^ m, t)
        copy.start()
        a_copies.append(copy)

    if relay:
        for j in range(2):
            master_copies[4, j] = master_relay(j, 1)
            master_copies[4, j].start()

    for d in range(depth):

        @pl.when(block(d) != f)
        def _(d=d):
            if d > 0:
                plane_copies[d].wait_recv()
            partner_copies[d].start()

    for d in range(depth):

        @pl.when(block(d) != f)
        def _(d=d):
            partner_copies[d].wait_recv()

    store = pltpu.make_async_copy(basis, basis_out, out_sem.at[0])
    store.start()
    for copy in a_copies:
        copy.wait_recv()

    high = min(rows, 256)
    for j in range(2):

        def add(i, total, j=j):
            update = jnp.dot(
                basis[j, at(i * high, high), :], ratio_ref[j], preferred_element_type=F32
            )
            return total + jnp.sum((update * update).reshape(high // 8, 8, width), axis=0)

        sums = lax.fori_loop(0, fs * rows // high, add, jnp.zeros((8, width), F32))
        sums = jnp.sum(sums, axis=0, keepdims=True)
        for h in range(width // HD):
            head = slice(h * HD, (h + 1) * HD)
            total = jnp.sum(sums[:, head], axis=1, keepdims=True)
            scale = 1.0 / jnp.sqrt(total / (fs * rows * HD) + norm_floor)
            scale_ref[j, :, head] = jnp.broadcast_to(scale, (8, HD))

    store.wait()
    kept.wait()
    early = {(1, 0), (2, 1)} if relay else set()
    for place, copy in master_copies.items():
        if place not in early:
            copy.wait_recv()
    for d in range(depth):

        @pl.when(block(d) != f)
        def _(d=d):
            partner_copies[d].wait_send()

    @pl.when(f != z)
    def _():
        for copy in plane_copies[1:]:
            copy.wait_send()

    @pl.when(f == z)
    def _():
        for m in direct:
            for j in range(2):
                basis_copies[m, j].wait_send()

    if relay:
        for j in range(2):

            @pl.when(f ^ (1 + j) == z)
            def _(j=j):
                basis_copies[3, j].wait_send()

    for copy in [swap] + z_copies:
        copy.wait_send()
    for copy in g_copies + forwards + r_copies + a_copies + list(master_copies.values()):
        copy.wait_send()


def final_kernel(*refs):
    scale_ref, ratio_ref, basis_ref, gathered_ref = refs[:4]
    inputs, moments, outs, moments_out = refs[4:8], refs[8:12], refs[12:18], refs[18:]
    for j in range(2):
        scale = scale_ref[j, 0:1, :]
        own_basis, master = inputs[2 * j : 2 * j + 2]
        step_out, weight_out, copy_out = outs[3 * j : 3 * j + 3]
        update = jnp.dot(own_basis[...], ratio_ref[j], preferred_element_type=F32)
        step = update * scale
        step_out[...] = step
        weight_out[...] = master[...] - step_rate * step
        update = jnp.dot(basis_ref[j], ratio_ref[j], preferred_element_type=F32)
        step = update * scale
        copy_out[...] = (gathered_ref[j].astype(F32) - step_rate * step).astype(BF)

    @pl.when(pl.program_id(0) == 0)
    def _():
        for source, target in zip(moments, moments_out):
            target[...] = source[...]


def body(fs, tp, *args):
    saved_input, query_cot, _, query_master, key_master, query_basis, key_basis = args[:7]
    rows, rank = query_basis.shape
    tokens, columns = saved_input.shape
    width = query_cot.shape[1]
    part = rank // fs
    depth = tp // 2
    count = fs * rows
    half, chunk = tokens // 2, tokens // tp
    any_spec = pl.BlockSpec(memory_space=pl.ANY)
    vmem = pl.BlockSpec(memory_space=pltpu.VMEM)
    dma = pltpu.SemaphoreType.DMA
    moment = jax.ShapeDtypeStruct((part, width), F32)
    pairs = []
    for shape in ((fs, 2), (depth,), (depth,), (), (depth,), (depth,), (depth,), (fs,), (fs,), (fs + 1, 2)):
        pairs += [dma(shape), dma(shape)]
    results = pl.pallas_call(
        functools.partial(exchange_kernel, fs, tp),
        name="exchange",
        out_shape=(
            moment,
            moment,
            moment,
            moment,
            jax.ShapeDtypeStruct((2, rank, width), BF),
            jax.ShapeDtypeStruct((2, 8, width), F32),
            jax.ShapeDtypeStruct((2, count, width), BF),
            jax.ShapeDtypeStruct((2, count, rank), BF),
        ),
        in_specs=[any_spec] * 7 + [vmem] * 4,
        out_specs=(vmem,) * 6 + (any_spec,) * 2,
        scratch_shapes=[
            pltpu.VMEM((2, count, rank), BF),
            pltpu.VMEM((tokens, columns), BF),
            pltpu.VMEM((2, tokens, width), BF),
            pltpu.VMEM((2, rows, width), F32),
            pltpu.VMEM((2, rows, width), BF),
            pltpu.VMEM((half, 2 * rank), BF),
            pltpu.VMEM((half, 2 * rank), BF),
            pltpu.VMEM((half, 2 * rank), F32),
            pltpu.VMEM((half, 2 * rank), BF),
            pltpu.VMEM((depth, chunk, 2 * rank), BF),
            pltpu.VMEM((tokens, 2 * rank), BF),
            pltpu.VMEM((2, rank, width), F32),
            pltpu.VMEM((2, rank, width), BF),
            pltpu.VMEM((fs, 2, part, width), BF),
            dma((7,)),
            *pairs,
            dma((2,)),
        ],
        compiler_params=pltpu.CompilerParams(
            collective_id=0, has_side_effects=True, vmem_limit_bytes=60 * 1024 * 1024
        ),
    )(*args)
    moments, (ratio, scale, gathered, basis) = results[:4], results[4:]

    steps = min(8, rows // 16)
    own_tile, tile = rows // steps, count // steps

    def row(i):
        return (i, 0)

    def pair(i):
        return (0, i, 0)

    def whole(i):
        return (0, 0, 0)

    own_spec = pl.BlockSpec((own_tile, width), row)
    full_spec = pl.BlockSpec((tile, width), row)
    basis_spec = pl.BlockSpec((own_tile, rank), row)
    moment_spec = pl.BlockSpec((part, width), lambda i: (0, 0))
    big = jax.ShapeDtypeStruct((rows, width), F32)
    copied = jax.ShapeDtypeStruct((count, width), BF)
    outs = pl.pallas_call(
        final_kernel,
        name="final",
        out_shape=(big, big, copied) * 2 + (moment,) * 4,
        grid=(steps,),
        in_specs=[
            pl.BlockSpec((2, 8, width), whole),
            pl.BlockSpec((2, rank, width), whole),
            pl.BlockSpec((2, tile, rank), pair),
            pl.BlockSpec((2, tile, width), pair),
            basis_spec,
            own_spec,
            basis_spec,
            own_spec,
        ]
        + [moment_spec] * 4,
        out_specs=(own_spec, own_spec, full_spec) * 2 + (moment_spec,) * 4,
        compiler_params=pltpu.CompilerParams(vmem_limit_bytes=60 * 1024 * 1024),
    )(scale, ratio, basis, gathered, query_basis, query_master, key_basis, key_master, *moments)
    return (*outs[:3], *outs[6:8], *outs[3:6], *outs[8:])


def solution(mesh):
    split, tall, wide = P("fs", "tp"), P("fs", None), P(None, "tp")
    outs = (split, split, wide, split, split)
    return jax.shard_map(
        functools.partial(body, mesh.shape["fs"], mesh.shape["tp"]),
        mesh=mesh,
        in_specs=(split,) * 5 + (tall, tall) + (split,) * 4,
        out_specs=outs + outs,
        check_vma=False,
    )
```
